256 devices in a mesh: sp: 64 (over z, x, core), tp: 4 (over y).
Axes of the slice: x: 4, y: 4, z: 8, core: 2. Of those that a mesh axis runs over, the one named last changes fastest.
Arguments:
- moe_input: bfloat16 [8192, 2048], P('sp'), may hold values from -6 to 6
- out_cotangent: bfloat16 [8192, 2048], P('sp'), may hold values from -16 to 16
- routes: int32 [8192, 2], P('sp'), may hold values from 0 to 15, all different within a row; in each aligned block of 128 rows (0 to 127, 128 to 255, ...) at most 16 rows name the same one
- route_weight: float32 [8192, 2], P('sp'), may hold values from 0.2 to 1
- w_gate: bfloat16 [64, 2048, 896], P('sp', None, 'tp'), may hold values from -0.125 to 0.125
- w_up: bfloat16 [64, 2048, 896], P('sp', None, 'tp'), may hold values from -0.125 to 0.125
- w_down: bfloat16 [64, 896, 2048], P('sp', 'tp'), may hold values from -0.09375 to 0.09375
- out_proj: bfloat16 [2048, 1024], P(None, 'tp'), may hold values from -0.243067956 to 0.243067956
- conv_out: bfloat16 [8192, 1024], P('sp', 'tp'), may hold values from -17 to 17
- glu_value: bfloat16 [8192, 1024], P('sp', 'tp'), may hold values from -6 to 6
- glu_gate: bfloat16 [8192, 1024], P('sp', 'tp'), may hold values from -9 to 9
- taps: float32 [31, 1024], P(None, 'tp'), may hold values from -1 to 1
- norm_gain: float32 [1024], P('tp'), may hold values from 0.1 to 1.9
Outputs:
- grad_gate: bfloat16 [64, 2048, 896], P('sp', None, 'tp')
- grad_up: bfloat16 [64, 2048, 896], P('sp', None, 'tp')
- grad_down: bfloat16 [64, 896, 2048], P('sp', 'tp')
- grad_proj: float32 [2048, 1024], P('sp', 'tp')
- grad_glu_value: bfloat16 [8192, 1024], P('sp', 'tp')
- grad_glu_gate: bfloat16 [8192, 1024], P('sp', 'tp')
The draws below stay inside these ranges and needn't reach their ends.
Inputs may be any that keep to these rules, and one draw needn't show every extreme that they name: `routes`: each token names two different experts. Within the 128 tokens of one index of sp no expert is named more than 16 times, a bound that some block reaches.
All inputs are finite; a program needn't handle non-finite values.
Results may differ from the reference program's by a relative error of at most 0.014.
Values may be sent and summed in bfloat16 or wider, within the bound.
No kernel may reach another device: no remote copies, remote signals or barrier semaphores. Data moves between devices by JAX's collectives and lax.ppermute only.
A program may use at most 128 MiB of HBM per device.

```python
import math
import jax
import jax.numpy as jnp
import numpy as np
from jax import lax

D = 2048
DB = 1024
FF = 3584
WIDTH = 31
SPAN = 4
TOK_DEV = 128
TOKENS = 8192
EXPERTS = 16
CAP = 16
N_SP = 64
N_TP = 4


def channel_profile(rough_key, lowest, highest):
    rising = jnp.exp(jnp.linspace(math.log(lowest), math.log(highest), DB)).astype(jnp.float32)
    rough = jnp.exp(jax.random.uniform(rough_key, (DB,), jnp.float32, -0.35, 0.35))
    return rising * rough


def draw_out_proj(key, part):
    base_key, rough_key = jax.random.split(jax.random.fold_in(key, 11), 2)
    profile = channel_profile(rough_key, 0.6, 1.8)
    values = jnp.clip(jax.random.normal(base_key, (D, DB), jnp.float32), -4.0, 4.0)
    return (values * profile[None, :] / math.sqrt(D)).astype(jnp.bfloat16)


def draw_conv_out(key, part):
    base_key, rough_key = jax.random.split(jax.random.fold_in(key, 23), 2)
    profile = channel_profile(rough_key, 0.5, 2.0)
    values = jnp.clip(jax.random.normal(base_key, (TOKENS, DB), jnp.float32), -4.0, 4.0)
    return (values * profile[None, :]).astype(jnp.bfloat16)


def raised(drawn, rng, source, target, shards_of, factor):
    def block_of(position):
        return (jnp.arange(drawn.shape[position]) // (drawn.shape[position] // shards_of)).reshape((-1,) + (1,) * (drawn.ndim - 1 - position))

    near = jax.random.permutation(rng, shards_of)[block_of(target)]
    other_side = (block_of(target) + shards_of // 2) % shards_of
    return jnp.where((block_of(source) == near) | (block_of(source) == other_side), factor * drawn, drawn)


def steps_of(key, shape, shards, low, top_value):
    gain, own = 1.0, jax.random.fold_in(key, 6)
    for position, parts in shards:
        draws = jnp.exp(jax.random.uniform(jax.random.fold_in(own, position), (parts,), jnp.float32, low / len(shards), top_value / len(shards)))
        gain = gain * jnp.repeat(draws, shape[position] // parts).reshape([-1 if axis == position else 1 for axis in range(len(shape))])
    return gain


def shared_out(key, own, number, rows, amount, top, reach, skew):
    sequence = jax.random.permutation(key, amount)
    heavy_load, common = portions_of(amount, rows * top, reach, skew, True), portions_of(amount, rows * top, reach, skew, False)
    places = jnp.arange(amount)

    def named(sizes, offset_by):
        used = int((sizes > 0).sum())
        fixed = max(1, used // 4)
        moved = fixed + (places - fixed + offset_by * (used - fixed)) % max(1, amount - fixed)
        return jnp.zeros((amount,), jnp.int32).at[sequence[jnp.where(places < fixed, places, moved)]].set(jnp.asarray(sizes, jnp.int32))

    sizes = jnp.where(number % 4 == 0, named(heavy_load, number // 4), named(common, number - number // 4 - 1))
    mixed = jax.random.permutation(jax.random.fold_in(own, 3), amount)
    donor, receiver = mixed[0:amount // 2 * 2:2], mixed[1:amount // 2 * 2:2]
    room = jnp.minimum(sizes[donor] - 1, reach - sizes[receiver]) // 2
    room = jnp.where((donor == sequence[0]) | (receiver == sequence[0]) | (sizes[receiver] == 0), 0, jnp.maximum(room, 0))
    moved = jax.random.randint(jax.random.fold_in(own, 4), (amount // 2,), 0, 1 << 20) % (room + 1)
    sizes = sizes.at[donor].add(-moved).at[receiver].add(moved)
    items = jnp.searchsorted(jnp.cumsum(sizes), jnp.arange(rows * top), side="right").astype(jnp.int32)
    listing = items.reshape(top, rows).T
    listing = listing[jax.random.permutation(jax.random.fold_in(own, 1), rows)]
    offset_by = jax.random.randint(jax.random.fold_in(own, 2), (rows, 1), 0, top)
    return jnp.take_along_axis(listing, (jnp.arange(top)[None, :] + offset_by) % top, axis=1)


def portions_of(count, total, most, slope, full):
    weights = [(1 << 20) // math.isqrt(standing ** slope) + 1 for standing in range(1, count + 1)]
    largest = most if full else min(most, max(-(-total // count), total * weights[0] // sum(weights)))
    least = 1 if total - largest >= count - 1 else 0
    holding, surplus = [largest] + [least] * (count - 1), total - largest - least * (count - 1)
    while surplus > 0:
        free = [i for i in range(1, count) if holding[i] < largest] or [i for i in range(1, count) if holding[i] < most]
        mass, remaining = sum([weights[i] for i in free]), surplus
        for i in free:
            extra = min(most - holding[i], max(1, remaining * weights[i] // mass), surplus)
            holding[i] = holding[i] + extra
            surplus = surplus - extra
    return np.array(holding)


def scatter_about(key, extent, scale, reach, shards=(), held_as=jnp.bfloat16):
    array = scale * jax.random.normal(key, extent, jnp.float32)
    if shards:
        array = array * steps_of(key, extent, shards, -0.22, 0.18)
    return jnp.clip(array, -reach, reach).astype(held_as)


def gaussian_with(own_key, extent, deviation, most, pieces, heavy, kind=jnp.bfloat16):
    result = deviation * jax.random.normal(own_key, extent, jnp.float32)
    if pieces:
        result = result * steps_of(own_key, extent, pieces, -0.22, 0.18)
    return jnp.clip(raised(result, jax.random.fold_in(own_key, 3), *heavy), -most, most).astype(kind)


def setup_inputs(seed: int = 0) -> dict:
    splits = jax.random.split(jax.random.key(seed), 14)
    moe_input = scatter_about(splits[0], (TOKENS, D), 1.0, 6.0, ((0, 64),))
    out_cotangent = gaussian_with(splits[1], (TOKENS, D), 1.0, 16.0, ((0, 64),), (0, 1, 64, 4.0))
    routes_keys = jax.random.split(jax.random.fold_in(splits[2], 1), TOKENS // TOK_DEV)
    routes_turns = jax.random.permutation(jax.random.fold_in(splits[2], 3), TOKENS // TOK_DEV)
    routes = jax.vmap(lambda own, number: shared_out(jax.random.fold_in(splits[2], 2), own, number, TOK_DEV, EXPERTS, 2, CAP, 0))(routes_keys, routes_turns).reshape((TOKENS, 2))
    route_weight = jnp.clip(0.2 + 0.8 * jax.random.uniform(splits[3], (TOKENS, 2), jnp.float32) ** steps_of(splits[3], (TOKENS, 2), ((0, 64),), -0.2, 0.2), 0.2, 1.0)
    w_gate = scatter_about(splits[4], (EXPERTS * SPAN, D, FF // SPAN), D ** -0.5, 0.125, ((0, 64), (2, 4)))
    w_up = scatter_about(splits[5], (EXPERTS * SPAN, D, FF // SPAN), D ** -0.5, 0.125, ((0, 64), (2, 4)))
    w_down = scatter_about(splits[6], (EXPERTS * SPAN, FF // SPAN, D), FF ** -0.5, 0.09375, ((0, 64), (1, 4)))
    out_proj = draw_out_proj(jax.random.fold_in(splits[13], 71), 0)
    conv_out = draw_conv_out(jax.random.fold_in(splits[13], 71), 0)
    glu_value = scatter_about(splits[9], (TOKENS, DB), 1.0, 6.0, ((0, 64), (1, 4)))
    glu_gate = scatter_about(splits[10], (TOKENS, DB), 1.5, 9.0, ((0, 64), (1, 4)))
    taps = scatter_about(splits[11], (WIDTH, DB), WIDTH ** -0.5, 1.0, ((1, 4),), jnp.float32)
    norm_gain = jnp.clip(1.0 + 0.18 * jax.random.normal(splits[12], (DB,), jnp.float32), 0.1, 1.9)
    return {"moe_input": moe_input, "out_cotangent": out_cotangent, "routes": routes, "route_weight": route_weight, "w_gate": w_gate, "w_up": w_up, "w_down": w_down, "out_proj": out_proj, "conv_out": conv_out, "glu_value": glu_value, "glu_gate": glu_gate, "taps": taps, "norm_gain": norm_gain}


def swish_slope(pre, sig):
    return sig * (1.0 + pre * (1.0 - sig))

def reference(moe_input, out_cotangent, routes, route_weight, w_gate, w_up, w_down, out_proj, conv_out, glu_value, glu_gate, taps, norm_gain):
    f32 = jnp.float32
    bf16 = jnp.bfloat16
    blocks = routes.reshape(N_SP, 2 * TOK_DEV)
    one_hot = (blocks[:, :, None] == jnp.arange(EXPERTS, dtype=jnp.int32)[None, None, :]).astype(jnp.int32)
    earlier = jnp.cumsum(one_hot, axis=1) - one_hot
    slot_index = lax.optimization_barrier(jnp.sum(earlier * one_hot, axis=2)).astype(jnp.int32)
    target = blocks * CAP + slot_index
    token_ids = jnp.arange(N_SP, dtype=jnp.int32)[:, None] * TOK_DEV + jnp.arange(2 * TOK_DEV, dtype=jnp.int32)[None, :] // 2
    matches = jnp.arange(EXPERTS * CAP, dtype=jnp.int32)[None, :, None] == target[:, None, :]
    source = lax.optimization_barrier(jnp.sum(jnp.where(matches, token_ids[:, None, :], 0), axis=2)).astype(jnp.int32)
    weights = lax.optimization_barrier(jnp.sum(jnp.where(matches, route_weight.reshape(N_SP, 1, 2 * TOK_DEV), 0.0), axis=2))
    filled = jnp.any(matches, axis=2)

    def by_expert(table):
        return jnp.transpose(table.reshape(N_SP, EXPERTS, CAP), (1, 0, 2)).reshape(EXPERTS, N_SP * CAP)
    ff_dev = FF // (SPAN * N_TP)
    contract_rows = (((0,), (0,)), ((), ()))

    def one_expert(inputs):
        expert, source_row, weight_row, filled_row = inputs
        expert_rows = jnp.where(filled_row[:, None], moe_input[source_row], jnp.zeros((), bf16))
        expert_cot = (weight_row[:, None] * out_cotangent[source_row].astype(f32)).astype(bf16)
        gate_w = jnp.transpose(lax.dynamic_slice_in_dim(w_gate, expert * SPAN, SPAN, 0), (1, 0, 2)).reshape(D, FF)
        up_w = jnp.transpose(lax.dynamic_slice_in_dim(w_up, expert * SPAN, SPAN, 0), (1, 0, 2)).reshape(D, FF)
        down_w = lax.dynamic_slice_in_dim(w_down, expert * SPAN, SPAN, 0).reshape(FF, D)
        gate_pre = jnp.dot(expert_rows, gate_w, preferred_element_type=f32)
        up_pre = jnp.dot(expert_rows, up_w, preferred_element_type=f32)
        gate_sig = jax.nn.sigmoid(gate_pre)
        hidden = (gate_pre * gate_sig * up_pre).astype(bf16)
        d_hidden = lax.dot_general(expert_cot, down_w, (((1,), (1,)), ((), ())), preferred_element_type=f32)
        grad_down = lax.dot_general(hidden, expert_cot, contract_rows, preferred_element_type=f32).astype(bf16)
        d_gate = (d_hidden * up_pre * swish_slope(gate_pre, gate_sig)).astype(bf16)
        d_up = (d_hidden * gate_pre * gate_sig).astype(bf16)
        grad_gate = lax.dot_general(expert_rows, d_gate, contract_rows, preferred_element_type=f32).astype(bf16)
        grad_up = lax.dot_general(expert_rows, d_up, contract_rows, preferred_element_type=f32).astype(bf16)
        row_count = expert_rows.shape[0]
        partial_value = jnp.einsum('rsjf,dsjf->sjrd', d_gate.reshape(row_count, SPAN, N_TP, ff_dev).astype(f32), gate_w.reshape(D, SPAN, N_TP, ff_dev).astype(f32))
        partial_value = partial_value + jnp.einsum('rsjf,dsjf->sjrd', d_up.reshape(row_count, SPAN, N_TP, ff_dev).astype(f32), up_w.reshape(D, SPAN, N_TP, ff_dev).astype(f32))
        partial_value = lax.optimization_barrier(partial_value.astype(bf16))
        span_part = lax.optimization_barrier(lax.optimization_barrier(jnp.sum(partial_value.astype(f32), axis=1)).astype(bf16))
        slot_grad = lax.optimization_barrier(jnp.sum(span_part.astype(f32), axis=0))
        gate_blocks = jnp.transpose(grad_gate.reshape(D, SPAN, FF // SPAN), (1, 0, 2))
        up_blocks = jnp.transpose(grad_up.reshape(D, SPAN, FF // SPAN), (1, 0, 2))
        down_blocks = grad_down.reshape(SPAN, FF // SPAN, D)
        return (gate_blocks, up_blocks, down_blocks, slot_grad)
    gate_all, up_all, down_all, slot_grads = lax.map(one_expert, (jnp.arange(EXPERTS, dtype=jnp.int32), by_expert(source), by_expert(weights), by_expert(filled)))
    grad_gate = gate_all.reshape(EXPERTS * SPAN, D, FF // SPAN)
    grad_up = up_all.reshape(EXPERTS * SPAN, D, FF // SPAN)
    grad_down = down_all.reshape(EXPERTS * SPAN, FF // SPAN, D)
    slot_table = slot_grads.reshape(EXPERTS, N_SP, CAP, D)
    per_route = slot_table[blocks, jnp.arange(N_SP, dtype=jnp.int32)[:, None], slot_index]
    moe_grad = lax.optimization_barrier(jnp.sum(per_route.reshape(TOKENS, 2, D), axis=1))
    resid_grad = (out_cotangent.astype(f32) + moe_grad).astype(bf16)
    conv_vals = conv_out.astype(f32)
    mean = lax.optimization_barrier(jnp.sum(conv_vals, axis=1, keepdims=True)) / DB
    square_mean = lax.optimization_barrier(jnp.sum(conv_vals * conv_vals, axis=1, keepdims=True)) / DB
    rstd = lax.rsqrt(square_mean - mean * mean + 1e-05)
    normed = (conv_vals - mean) * rstd
    zpre = normed * norm_gain[None, :]
    zsig = jax.nn.sigmoid(zpre)
    mixed = (zpre * zsig).astype(bf16)
    grad_proj = lax.dot_general(resid_grad, mixed, contract_rows, preferred_element_type=f32)
    d_mixed = jnp.dot(resid_grad, out_proj, preferred_element_type=f32)
    d_norm = d_mixed * swish_slope(zpre, zsig) * norm_gain[None, :]
    first_sum = lax.optimization_barrier(jnp.sum(d_norm, axis=1, keepdims=True)) / DB
    second_sum = lax.optimization_barrier(jnp.sum(d_norm * normed, axis=1, keepdims=True)) / DB
    conv_grad = (rstd * (d_norm - first_sum - normed * second_sum)).astype(bf16)
    extended = jnp.pad(conv_grad.astype(f32), ((0, WIDTH - 1), (0, 0)))
    unit_grad = lax.conv_general_dilated(extended[None], taps[:, None, :], (1,), 'VALID', dimension_numbers=('NWC', 'WIO', 'NWC'), feature_group_count=DB, precision=lax.Precision.HIGHEST)[0]
    gate_sig_in = jax.nn.sigmoid(glu_gate.astype(f32))
    grad_glu_value = (unit_grad * gate_sig_in).astype(bf16)
    grad_glu_gate = (unit_grad * glu_value.astype(f32) * gate_sig_in * (1.0 - gate_sig_in)).astype(bf16)
    return (grad_gate, grad_up, grad_down, grad_proj, grad_glu_value, grad_glu_gate)
```

```python
import jax
import jax.numpy as jnp
from jax import lax
from jax.experimental import pallas as pl
from jax.experimental.pallas import tpu as pltpu
from jax.sharding import Mesh, PartitionSpec as P

DB = 1024
WIDTH = 31
EXPERTS = 16
CAP = 16
NZ, NX, NC, NY = 8, 4, 2, 4
ZX = NZ * NX
SP = ("z", "x", "c")
F32 = jnp.float32
BF16 = jnp.bfloat16


VMEM = pl.BlockSpec(memory_space=pltpu.VMEM)
SMEM = pl.BlockSpec(memory_space=pltpu.SMEM)
CONTRACT_FIRST = (((0,), (0,)), ((), ()))
CONTRACT_LAST = (((1,), (1,)), ((), ()))


def to_y(v, d):
    return lax.ppermute(v, "y", [(i, (i + d) % NY) for i in range(NY)])


def to_x(v):
    return lax.ppermute(v, "x", [(i, i ^ 1) for i in range(NX)])


def to_xy(v, d):
    pairs = [(x * NY + i, (x ^ 1) * NY + (i + d) % NY) for x in range(NX) for i in range(NY)]
    return lax.ppermute(v, ("x", "y"), pairs)


def to_c(v):
    return lax.ppermute(v, "c", [(0, 1), (1, 0)])


def swish_slope(pre, sig):
    return sig * (1.0 + pre * (1.0 - sig))


def prep_body(routes, weights, rows, cots, send, places):
    lane = lax.broadcasted_iota(jnp.int32, (EXPERTS, 128), 0)
    first = (lane == routes[0:1, :]).astype(F32)
    second = (lane == routes[1:2, :]).astype(F32)
    before = (
        lax.broadcasted_iota(jnp.int32, (128, 128), 0)
        < lax.broadcasted_iota(jnp.int32, (128, 128), 1)
    ).astype(BF16)
    earlier = jnp.dot((first + second).astype(BF16), before, preferred_element_type=F32)
    slot0 = jnp.sum(earlier * first, axis=0, keepdims=True).astype(jnp.int32)
    slot1 = jnp.sum(earlier * second, axis=0, keepdims=True).astype(jnp.int32)
    place = lax.broadcasted_iota(jnp.int32, (EXPERTS * CAP, 128), 0)
    hit0 = place == routes[0:1, :] * CAP + slot0
    hit1 = place == routes[1:2, :] * CAP + slot1
    scale = jnp.sum(
        jnp.where(hit0, weights[0:1, :], 0.0) + jnp.where(hit1, weights[1:2, :], 0.0),
        axis=1,
        keepdims=True,
    )
    pick = jnp.where(hit0 | hit1, 1.0, 0.0).astype(BF16)
    places[...] = pick
    sent_rows = jnp.dot(pick, rows[...], preferred_element_type=F32).astype(BF16)
    sent_cots = (scale * jnp.dot(pick, cots[...], preferred_element_type=F32)).astype(BF16)
    for half in range(2):
        cols = slice(256 * half, 256 * half + 256)
        send[:, half, 0] = sent_rows[:, cols].reshape(EXPERTS, CAP, 256)
        send[:, half, 1] = sent_cots[:, cols].reshape(EXPERTS, CAP, 256)


def prep(routes, weights, rows, cots):
    return pl.pallas_call(
        prep_body,
        out_shape=(
            jax.ShapeDtypeStruct((EXPERTS, 2, 2, CAP, 256), BF16),
            jax.ShapeDtypeStruct((EXPERTS * CAP, 128), BF16),
        ),
        in_specs=[VMEM] * 4,
        out_specs=(VMEM, VMEM),
        name="prep",
    )(routes, weights, rows, cots)


PIECES = (
    (0, 0, 0, 32),
    (0, 3, 0, 32),
    (0, 1, 0, 32),
    (1, 0, 0, 32),
    (1, 3, 0, 16),
    (1, 3, 16, 16),
    (1, 1, 0, 16),
    (1, 1, 16, 16),
    (0, 2, 0, 16),
    (0, 2, 16, 16),
    (1, 2, 0, 10),
    (1, 2, 10, 6),
    (1, 2, 16, 6),
    (1, 2, 22, 10),
)


def gather_pieces(v):
    h = ZX // 2
    behind, ahead, beside = to_y(v, 1), to_y(v, -1), to_x(v)
    side_behind_hi = to_y(beside[h:], 1)
    side_ahead_lo = to_y(beside[:h], -1)
    side_behind_lo = to_x(behind[:h])
    side_ahead_hi = to_x(ahead[h:])
    far_lo = to_y(behind[:h], 1)
    far_hi = to_y(ahead[h:], -1)
    t = 10
    last = (
        to_y(side_behind_lo[:t], 1),
        to_x(far_lo[t:]),
        to_x(far_hi[: h - t]),
        to_y(side_ahead_hi[h - t :], -1),
    )
    return (
        v,
        behind,
        ahead,
        beside,
        side_behind_lo,
        side_behind_hi,
        side_ahead_lo,
        side_ahead_hi,
        far_lo,
        far_hi,
        *last,
    )


def rows_body(cols, *refs):
    pieces = refs[: len(PIECES)]
    w_gate, w_up, w_down = refs[len(PIECES) : len(PIECES) + 3]
    rows, cots, act, d_gate, d_up = refs[len(PIECES) + 3 : len(PIECES) + 8]
    grads = refs[len(PIECES) + 8 :]
    for piece, (dx, dy, first, count) in zip(pieces, PIECES):
        at = pl.ds(pl.multiple_of(cols[4 * dx + dy], 256), 256)
        span = slice(first * CAP, (first + count) * CAP)
        rows[span, at] = piece[:, 0].reshape(count * CAP, 256)
        cots[span, at] = piece[:, 1].reshape(count * CAP, 256)
    for m in range(2):
        span = slice(256 * m, 256 * m + 256)
        gate = lax.dot_general(rows[span], w_gate[...], CONTRACT_LAST, preferred_element_type=F32)
        up = lax.dot_general(rows[span], w_up[...], CONTRACT_LAST, preferred_element_type=F32)
        d_act = lax.dot_general(cots[span], w_down[...], CONTRACT_LAST, preferred_element_type=F32)
        sig = jax.nn.sigmoid(gate)
        silu = gate * sig
        act[span] = (silu * up).astype(BF16)
        d_gate[span] = (d_act * up * swish_slope(gate, sig)).astype(BF16)
        d_up[span] = (d_act * silu).astype(BF16)
    for i, grad in enumerate(grads):
        at = pl.ds(pl.multiple_of(cols[i], 256), 256)
        part = jnp.dot(d_gate[...], w_gate[:, at], preferred_element_type=F32) + jnp.dot(
            d_up[...], w_up[:, at], preferred_element_type=F32
        )
        grad[...] = part.astype(BF16).reshape(ZX, CAP, 256)


def expert_rows_pass(cols, pieces, w_gate, w_up, w_down):
    n, d = ZX * CAP, w_gate.shape[1]
    units = w_gate.shape[0]
    return pl.pallas_call(
        rows_body,
        out_shape=(jax.ShapeDtypeStruct((n, d), BF16),) * 2
        + (jax.ShapeDtypeStruct((n, units), BF16),) * 3
        + (jax.ShapeDtypeStruct((ZX, CAP, 256), BF16),) * 8,
        in_specs=[SMEM] + [VMEM] * (len(PIECES) + 3),
        out_specs=(VMEM,) * 13,
        name="expert_rows",
    )(cols, *pieces, w_gate, w_up, w_down)


def weights_body(rows, cots, act, d_gate, d_up, *outs):
    half = act.shape[1] // 2
    for i, (left, right) in enumerate(((d_gate, rows), (d_up, rows), (act, cots))):
        for n in range(4):
            at = slice(512 * n, 512 * n + 512)
            grad = lax.dot_general(
                left[...], right[:, at], CONTRACT_FIRST, preferred_element_type=F32
            ).astype(BF16)
            outs[i][:, at] = grad[:half]
            outs[3 + i][:, at] = grad[half:]


def expert_weights_pass(rows, cots, act, d_gate, d_up):
    out = jax.ShapeDtypeStruct((act.shape[1] // 2, rows.shape[1]), BF16)
    return pl.pallas_call(
        weights_body,
        out_shape=(out,) * 6,
        in_specs=[VMEM] * 5,
        out_specs=(VMEM,) * 6,
        name="expert_weights",
    )(rows, cots, act, d_gate, d_up)


def combine_body(returned, places, cot, out):
    for half in range(2):
        cols = slice(256 * half, 256 * half + 256)
        slots = returned[:, half].reshape(EXPERTS * CAP, 256)
        moe = lax.dot_general(places[...], slots, CONTRACT_FIRST, preferred_element_type=F32)
        out[:, cols] = (cot[:, cols].astype(F32) + moe).astype(BF16)


def combine(returned, places, cot):
    return pl.pallas_call(
        combine_body,
        out_shape=jax.ShapeDtypeStruct(cot.shape, BF16),
        in_specs=[VMEM] * 3,
        out_specs=VMEM,
        name="combine",
    )(returned, places, cot)


def proj_body(where, own, one, two, three, mixed, resid, keep, send, table):
    for d, piece in enumerate((own, one, two, three)):
        block = lax.rem(where[0] + (NY - d), NY)
        resid[:, pl.ds(pl.multiple_of(block * 512, 512), 512)] = piece[...]
        part = lax.dot_general(piece[...], mixed[...], CONTRACT_FIRST, preferred_element_type=F32)
        table[pl.ds(block * 16, 16)] = part.reshape(16, 32, 256)
    core = where[1]
    for i in range(ZX):
        keep[i] = table[2 * i + core]
        send[i] = table[2 * i + 1 - core].astype(BF16)


def proj(where, pieces, mixed):
    return pl.pallas_call(
        proj_body,
        out_shape=(
            jax.ShapeDtypeStruct((128, 2048), BF16),
            jax.ShapeDtypeStruct((ZX, 32, 256), F32),
            jax.ShapeDtypeStruct((ZX, 32, 256), BF16),
        ),
        in_specs=[SMEM] + [VMEM] * 5,
        out_specs=(VMEM,) * 3,
        scratch_shapes=[pltpu.VMEM((64, 32, 256), F32)],
        name="proj",
    )(where, *pieces, mixed)


def sum_over_y(v):
    return v + to_y(v, 1) + to_y(v, -1) + to_y(v, 2)


def local(
    moe_input,
    out_cotangent,
    routes,
    route_weight,
    w_gate,
    w_up,
    w_down,
    out_proj,
    conv_out,
    glu_value,
    glu_gate,
    taps,
    norm_gain,
):
    y = lax.axis_index("y")
    x_low = lax.axis_index("x") % 2
    core = lax.axis_index("c")
    quarter = moe_input.shape[1] // NY
    own_rows = lax.dynamic_slice_in_dim(moe_input, y * quarter, quarter, 1)
    own_cot = lax.dynamic_slice_in_dim(out_cotangent, y * quarter, quarter, 1)
    send, places = prep(routes.T, route_weight.T, own_rows, own_cot)
    shard = lax.all_to_all(send.reshape(ZX, 2, CAP, 256), ("z", "x"), 0, 0, tiled=True)
    pieces = gather_pieces(shard)

    own_w = (w_gate[0].T, w_up[0].T, w_down[0])
    both_w = [jnp.concatenate([w, to_c(w)], axis=0) for w in own_w]
    cols = jnp.stack(
        [256 * (2 * ((y + dy) % NY) + (x_low ^ dx)) for dx in range(2) for dy in range(NY)]
    ).astype(jnp.int32)
    rows, cots, act, d_gate, d_up, *parts = expert_rows_pass(cols, pieces, *both_w)
    total = parts[0].astype(F32)
    arrived = (
        to_xy(parts[5], 1),
        to_xy(parts[7], -1),
        to_y(parts[2], 2),
        to_xy(parts[6], 2),
        to_y(parts[1], 1),
        to_y(parts[3], -1),
        to_x(parts[4]),
    )
    for part in arrived:
        total = total + part.astype(F32)
    returned = lax.all_to_all(total.astype(BF16), ("z", "x"), 0, 0, tiled=True)
    resid_part = combine(returned.reshape(EXPERTS, 2, CAP, 256), places, own_cot)
    resid_pieces = (resid_part, to_y(resid_part, 1), to_y(resid_part, 2), to_y(resid_part, 3))

    weight_grads = expert_weights_pass(rows, cots, act, d_gate, d_up)
    grad_gate, grad_up, grad_down = [
        (own.astype(F32) + to_c(other).astype(F32)).astype(BF16)
        for own, other in zip(weight_grads[:3], weight_grads[3:])
    ]

    conv_vals = conv_out.astype(F32)
    sums = sum_over_y(
        jnp.stack([jnp.sum(conv_vals, axis=1), jnp.sum(conv_vals * conv_vals, axis=1)])
    )
    mean = sums[0][:, None] / DB
    rstd = lax.rsqrt(sums[1][:, None] / DB - mean * mean + 1e-05)
    normed = (conv_vals - mean) * rstd
    zpre = normed * norm_gain[None, :]
    zsig = jax.nn.sigmoid(zpre)
    mixed = (zpre * zsig).astype(BF16)

    resid_grad, keep, give = proj(jnp.stack([y, core]).astype(jnp.int32), resid_pieces, mixed)
    by_owner = (keep + to_c(give).astype(F32)).astype(BF16)
    grad_proj = jnp.sum(
        lax.all_to_all(by_owner, ("z", "x"), 0, 0, tiled=True).astype(F32), axis=0
    )

    d_mixed = jnp.dot(resid_grad, out_proj, preferred_element_type=F32)
    d_norm = d_mixed * swish_slope(zpre, zsig) * norm_gain[None, :]
    sums = sum_over_y(jnp.stack([jnp.sum(d_norm, axis=1), jnp.sum(d_norm * normed, axis=1)]))
    conv_grad = (
        rstd * (d_norm - sums[0][:, None] / DB - normed * sums[1][:, None] / DB)
    ).astype(BF16)
    n_sp = NZ * NX * NC
    later_rows = lax.ppermute(conv_grad[: WIDTH - 1], SP, [(i, i - 1) for i in range(1, n_sp)])
    extended = jnp.concatenate([conv_grad, later_rows], axis=0).astype(F32)
    unit_grad = lax.conv_general_dilated(
        extended[None],
        taps[:, None, :],
        (1,),
        "VALID",
        dimension_numbers=("NWC", "WIO", "NWC"),
        feature_group_count=taps.shape[1],
        precision=lax.Precision.HIGHEST,
    )[0]
    gate_sig_in = jax.nn.sigmoid(glu_gate.astype(F32))
    grad_glu_value = (unit_grad * gate_sig_in).astype(BF16)
    grad_glu_gate = (
        unit_grad * glu_value.astype(F32) * gate_sig_in * (1.0 - gate_sig_in)
    ).astype(BF16)
    return (
        grad_gate.T[None],
        grad_up.T[None],
        grad_down[None],
        grad_proj,
        grad_glu_value,
        grad_glu_gate,
    )


def solution(mesh):
    wide = Mesh(mesh.devices.reshape(NZ, NX, NC, NY), ("z", "x", "c", "y"))
    in_specs = (
        P(SP, None),
        P(SP, None),
        P(SP, None),
        P(SP, None),
        P(SP, None, "y"),
        P(SP, None, "y"),
        P(SP, "y", None),
        P(None, "y"),
        P(SP, "y"),
        P(SP, "y"),
        P(SP, "y"),
        P(None, "y"),
        P("y"),
    )
    out_specs = (
        P(SP, None, "y"),
        P(SP, None, "y"),
        P(SP, "y", None),
        P(SP, "y"),
        P(SP, "y"),
        P(SP, "y"),
    )
    return jax.shard_map(local, mesh=wide, in_specs=in_specs, out_specs=out_specs, check_vma=False)
```

```python
import jax
import jax.numpy as jnp
from jax import lax
from jax.experimental import pallas as pl
from jax.experimental.pallas import tpu as pltpu
from jax.sharding import Mesh, PartitionSpec as P


DB = 1024
WIDTH = 31
EXPERTS = 16
CAP = 16
NZ, NX, NC, NY = 8, 4, 2, 4
ZX = NZ * NX
SP = ("z", "x", "c")
F32 = jnp.float32
BF16 = jnp.bfloat16


VMEM = pl.BlockSpec(memory_space=pltpu.VMEM)
HBM = pl.BlockSpec(memory_space=pl.ANY)
CONTRACT_FIRST = (((0,), (0,)), ((), ()))
CONTRACT_LAST = (((1,), (1,)), ((), ()))


def to_y(v, d):
    return lax.ppermute(v, "y", [(i, (i + d) % NY) for i in range(NY)])


def to_x(v):
    return lax.ppermute(v, "x", [(i, i ^ 1) for i in range(NX)])


def to_xy(v, d):
    pairs = [(x * NY + i, (x ^ 1) * NY + (i + d) % NY) for x in range(NX) for i in range(NY)]
    return lax.ppermute(v, ("x", "y"), pairs)


def to_c(v):
    return lax.ppermute(v, "c", [(0, 1), (1, 0)])


def swish_slope(pre, sig):
    return sig * (1.0 + pre * (1.0 - sig))


def own_col(dx, dy):
    block = lax.rem(lax.axis_index("y") + dy, NY)
    return 256 * (2 * block + lax.rem(lax.axis_index("x") + dx, 2))


def own_quarter():
    return pl.ds(pl.multiple_of(512 * lax.axis_index("y"), 512), 512)


def prep_body(routes, weights, all_rows, all_cots, send, places, own_cot, rows, cots, sems):
    copies = [
        pltpu.make_async_copy(src.at[:, own_quarter()], dst, sems.at[i])
        for i, (src, dst) in enumerate(((all_rows, rows), (all_cots, cots)))
    ]
    for copy in copies:
        copy.start()
    lane = lax.broadcasted_iota(jnp.int32, (EXPERTS, 128), 0)
    first = (lane == routes[0:1, :]).astype(F32)
    second = (lane == routes[1:2, :]).astype(F32)
    before = (
        lax.broadcasted_iota(jnp.int32, (128, 128), 0)
        < lax.broadcasted_iota(jnp.int32, (128, 128), 1)
    ).astype(BF16)
    earlier = jnp.dot((first + second).astype(BF16), before, preferred_element_type=F32)
    slot0 = jnp.sum(earlier * first, axis=0, keepdims=True).astype(jnp.int32)
    slot1 = jnp.sum(earlier * second, axis=0, keepdims=True).astype(jnp.int32)
    place = lax.broadcasted_iota(jnp.int32, (EXPERTS * CAP, 128), 0)
    hit0 = place == routes[0:1, :] * CAP + slot0
    hit1 = place == routes[1:2, :] * CAP + slot1
    scale = jnp.sum(
        jnp.where(hit0, weights[0:1, :], 0.0) + jnp.where(hit1, weights[1:2, :], 0.0),
        axis=1,
        keepdims=True,
    )
    pick = jnp.where(hit0 | hit1, 1.0, 0.0).astype(BF16)
    places[...] = pick
    for copy in copies:
        copy.wait()
    own_cot[...] = cots[...]
    sent_rows = jnp.dot(pick, rows[...], preferred_element_type=F32).astype(BF16)
    sent_cots = (scale * jnp.dot(pick, cots[...], preferred_element_type=F32)).astype(BF16)
    for half in range(2):
        cols = slice(256 * half, 256 * half + 256)
        send[:, half, 0] = sent_rows[:, cols].reshape(EXPERTS, CAP, 256)
        send[:, half, 1] = sent_cots[:, cols].reshape(EXPERTS, CAP, 256)


def prep(routes, weights, rows, cots):
    return pl.pallas_call(
        prep_body,
        out_shape=(
            jax.ShapeDtypeStruct((EXPERTS, 2, 2, CAP, 256), BF16),
            jax.ShapeDtypeStruct((EXPERTS * CAP, 128), BF16),
            jax.ShapeDtypeStruct((128, 512), BF16),
        ),
        in_specs=[VMEM, VMEM, HBM, HBM],
        out_specs=(VMEM,) * 3,
        scratch_shapes=[
            pltpu.VMEM((128, 512), BF16),
            pltpu.VMEM((128, 512), BF16),
            pltpu.SemaphoreType.DMA((2,)),
        ],
        name="prep",
    )(routes, weights, rows, cots)


BLOCKS = ((0, 0), (0, 3), (0, 1), (1, 0), (1, 3), (1, 1), (0, 2), (1, 2))
STAGES = ((0, 4), (4, 7), (7, 8))
HALF = ZX // 2
LAYOUTS = (
    ((0, 0, ZX), (1, 0, ZX), (2, 0, ZX), (3, 0, ZX)),
    ((0, 0, ZX), (1, 0, ZX), (2, 0, ZX)),
    ((0, 0, HALF), (0, HALF, HALF)),
)


def gather_first(v):
    return v, to_y(v, 1), to_y(v, -1), to_x(v)


def gather_second(first):
    _, behind, _, beside = first
    return to_x(behind), to_y(beside, -1), to_y(behind, 1)


def gather_third(second):
    return to_y(second[0][:HALF], 1), to_y(second[1][HALF:], -1)


def weights_in_order_body(*refs):
    for i in range(3):
        for stage, (lo, hi) in enumerate(STAGES):
            out = refs[6 + 3 * i + stage]
            for block in range(lo, hi):
                at = pl.ds(pl.multiple_of(own_col(*BLOCKS[block]), 256), 256)
                cols = slice(256 * (block - lo), 256 * (block - lo + 1))
                for side in range(2):
                    out[224 * side : 224 * side + 224, cols] = refs[2 * i + side][:, at]


def weights_in_order(flat):
    out = tuple(jax.ShapeDtypeStruct((448, 256 * (hi - lo)), BF16) for lo, hi in STAGES)
    res = pl.pallas_call(
        weights_in_order_body,
        out_shape=out * 3,
        in_specs=[VMEM] * 6,
        out_specs=(VMEM,) * 9,
        name="weights_in_order",
    )(*flat)
    return [(res[s], res[3 + s], res[6 + s]) for s in range(3)]


def put_pieces(pieces, layout, rows, cots):
    for piece, (block, first, count) in zip(pieces, layout):
        cols = slice(256 * block, 256 * block + 256)
        span = slice(first * CAP, (first + count) * CAP)
        rows[span, cols] = piece[:, 0].reshape(count * CAP, 256)
        cots[span, cols] = piece[:, 1].reshape(count * CAP, 256)


def stage_pass(stage, pieces, weights, before):
    layout = LAYOUTS[stage]
    n = len(layout)
    width = 256 * (STAGES[stage][1] - STAGES[stage][0])

    def body(*refs):
        given = refs[n + 3 : n + 3 + len(before)]
        rows, cots, *sums = refs[n + 3 + len(before) :]
        put_pieces(refs[:n], layout, rows, cots)
        for i, left in enumerate((rows, rows, cots)):
            part = lax.dot_general(
                left[...], refs[n + i][...], CONTRACT_LAST, preferred_element_type=F32
            )
            sums[i][...] = part + given[i][...] if before else part

    return pl.pallas_call(
        body,
        out_shape=(jax.ShapeDtypeStruct((ZX * CAP, width), BF16),) * 2
        + (jax.ShapeDtypeStruct((ZX * CAP, 448), F32),) * 3,
        in_specs=[VMEM] * (n + 3 + len(before)),
        out_specs=(VMEM,) * 5,
        input_output_aliases={n + 3 + i: 2 + i for i in range(len(before))},
    )(*pieces, *weights, *before)


def weights_of(block, gates):
    stage = next(s for s, (lo, hi) in enumerate(STAGES) if lo <= block < hi)
    at = 256 * (block - STAGES[stage][0])
    return gates[stage][:, at : at + 256]


def row_grads(d_gate, d_up, gate_w, up_w, blocks, grads):
    for block, grad in zip(blocks, grads):
        part = jnp.dot(
            d_gate[...], weights_of(block, gate_w), preferred_element_type=F32
        ) + jnp.dot(d_up[...], weights_of(block, up_w), preferred_element_type=F32)
        grad[...] = part.astype(BF16).reshape(ZX, CAP, 256)


FAR = (5, 4, 6, 7)
NEAR = (2, 1, 3, 0)


def last_body(*refs):
    pieces = refs[:2]
    gate_w, up_w, down_w = refs[2:5], refs[5:8], refs[8]
    before = refs[9:12]
    rows, cots, act, d_gate, d_up = refs[12:17]
    put_pieces(pieces, LAYOUTS[2], rows, cots)

    @pl.loop(0, 2)
    def _(m):
        span = pl.ds(pl.multiple_of(256 * m, 256), 256)
        gate, up, d_act = [
            before[i][span]
            + lax.dot_general(left[span], w[...], CONTRACT_LAST, preferred_element_type=F32)
            for i, (left, w) in enumerate(((rows, gate_w[2]), (rows, up_w[2]), (cots, down_w)))
        ]
        sig = jax.nn.sigmoid(gate)
        silu = gate * sig
        act[span] = (silu * up).astype(BF16)
        d_gate[span] = (d_act * up * swish_slope(gate, sig)).astype(BF16)
        d_up[span] = (d_act * silu).astype(BF16)

    row_grads(d_gate, d_up, gate_w, up_w, FAR, refs[17:21])


def last_pass(pieces, gate_w, up_w, down_w, before):
    n = ZX * CAP
    return pl.pallas_call(
        last_body,
        out_shape=(jax.ShapeDtypeStruct((n, 256), BF16),) * 2
        + (jax.ShapeDtypeStruct((n, 448), BF16),) * 3
        + (jax.ShapeDtypeStruct((ZX, CAP, 256), BF16),) * 4,
        in_specs=[VMEM] * 12,
        out_specs=(VMEM,) * 9,
        name="last_stage",
    )(*pieces, *gate_w, *up_w, down_w, *before)


def near_body(*refs):
    row_grads(refs[0], refs[1], refs[2:5], refs[5:8], NEAR, refs[8:12])


def near_pass(d_gate, d_up, gate_w, up_w):
    return pl.pallas_call(
        near_body,
        out_shape=(jax.ShapeDtypeStruct((ZX, CAP, 256), BF16),) * 4,
        in_specs=[VMEM] * 8,
        out_specs=(VMEM,) * 4,
        name="near_rows",
    )(d_gate, d_up, *gate_w, *up_w)


def weights_body(*refs):
    rows, cots = refs[0:3], refs[3:6]
    act, d_gate, d_up = refs[6:9]
    outs = refs[9:15]
    turned = refs[15]
    half = 224
    for i, (left, rights) in enumerate(((d_gate, rows), (d_up, rows), (act, cots))):
        turned[...] = left[...].T
        for stage, (lo, hi) in enumerate(STAGES):
            for block in range(lo, hi):
                at = slice(256 * (block - lo), 256 * (block - lo + 1))
                grad = jnp.dot(turned[...], rights[stage][:, at], preferred_element_type=F32)
                grad = grad.astype(BF16)
                to = pl.ds(pl.multiple_of(own_col(*BLOCKS[block]), 256), 256)
                outs[i][:, to] = grad[:half]
                outs[3 + i][:, to] = grad[half:]


def expert_weights_pass(rows, cots, act, d_gate, d_up):
    out = jax.ShapeDtypeStruct((act.shape[1] // 2, 2048), BF16)
    return pl.pallas_call(
        weights_body,
        out_shape=(out,) * 6,
        in_specs=[VMEM] * 9,
        out_specs=(VMEM,) * 6,
        scratch_shapes=[pltpu.VMEM((448, ZX * CAP), BF16)],
        name="expert_weights",
    )(*rows, *cots, act, d_gate, d_up)


def finish_body(*refs):
    for i in range(3):
        total = refs[i][...].astype(F32) + refs[3 + i][...].astype(F32)
        refs[6 + i][...] = total.astype(BF16)


def finish(own, others):
    out = jax.ShapeDtypeStruct(own[0].shape, BF16)
    return pl.pallas_call(
        finish_body,
        out_shape=(out,) * 3,
        in_specs=[VMEM] * 6,
        out_specs=(VMEM,) * 3,
        name="finish",
    )(*own, *others)


def combine_body(returned, places, cot, out):
    for half in range(2):
        cols = slice(256 * half, 256 * half + 256)
        slots = returned[:, half].reshape(EXPERTS * CAP, 256)
        moe = lax.dot_general(places[...], slots, CONTRACT_FIRST, preferred_element_type=F32)
        out[:, cols] = (cot[:, cols].astype(F32) + moe).astype(BF16)


def combine(returned, places, cot):
    return pl.pallas_call(
        combine_body,
        out_shape=jax.ShapeDtypeStruct(cot.shape, BF16),
        in_specs=[VMEM] * 3,
        out_specs=VMEM,
        name="combine",
    )(returned, places, cot)


def proj_body(own, one, two, three, mixed, resid, keep, send, table):
    y = lax.axis_index("y")
    for d, piece in enumerate((own, one, two, three)):
        block = lax.rem(y + (NY - d), NY)
        resid[:, pl.ds(pl.multiple_of(block * 512, 512), 512)] = piece[...]
        part = lax.dot_general(piece[...], mixed[...], CONTRACT_FIRST, preferred_element_type=F32)
        table[pl.ds(block * 8, 8)] = part.astype(BF16).reshape(8, 2, 32, 256)
    core = lax.axis_index("c")
    keep[...] = table[:, core]
    send[...] = table[:, 1 - core]


def proj(pieces, mixed):
    return pl.pallas_call(
        proj_body,
        out_shape=(
            jax.ShapeDtypeStruct((128, 2048), BF16),
            jax.ShapeDtypeStruct((ZX, 32, 256), BF16),
            jax.ShapeDtypeStruct((ZX, 32, 256), BF16),
        ),
        in_specs=[VMEM] * 5,
        out_specs=(VMEM,) * 3,
        scratch_shapes=[pltpu.VMEM((ZX, 2, 32, 256), BF16)],
        name="proj",
    )(*pieces, mixed)


def channels_body(resid, out_proj, normed, gain, d_norm, sums):
    d_mixed = jnp.dot(resid[...], out_proj[...], preferred_element_type=F32)
    zpre = normed[...] * gain[...]
    grad = d_mixed * swish_slope(zpre, jax.nn.sigmoid(zpre)) * gain[...]
    d_norm[...] = grad
    first = jnp.sum(grad, axis=1, keepdims=True)
    second = jnp.sum(grad * normed[...], axis=1, keepdims=True)
    lane = lax.broadcasted_iota(jnp.int32, (128, 128), 1)
    table = jnp.where(lane == 0, first, jnp.where(lane == 1, second, 0.0))
    sums[...] = table.T[0:8]


def channels(resid, out_proj, normed, gain):
    return pl.pallas_call(
        channels_body,
        out_shape=(
            jax.ShapeDtypeStruct(normed.shape, F32),
            jax.ShapeDtypeStruct((8, 128), F32),
        ),
        in_specs=[VMEM] * 4,
        out_specs=(VMEM,) * 2,
        name="channels",
    )(resid, out_proj, normed, gain)


def sum_over_y(v):
    return v + to_y(v, 1) + to_y(v, -1) + to_y(v, 2)


def step(
    moe_input,
    out_cotangent,
    routes,
    route_weight,
    w_gate,
    w_up,
    w_down,
    out_proj,
    conv_out,
    glu_value,
    glu_gate,
    taps,
    norm_gain,
):
    send, places, own_cot = prep(routes.T, route_weight.T, moe_input, out_cotangent)
    shard = lax.all_to_all(send.reshape(ZX, 2, CAP, 256), ("z", "x"), 0, 0, tiled=True)
    own_w = (w_gate[0].T, w_up[0].T, w_down[0])
    ordered = weights_in_order([v for w in own_w for v in (w, to_c(w))])
    shard, ordered = lax.optimization_barrier((shard, ordered))
    gate_w, up_w, down_w = zip(*ordered)
    first = gather_first(shard)
    second = gather_second(first)
    rows0, cots0, *sums = stage_pass(0, first, ordered[0], ())
    third = gather_third(second)
    rows1, cots1, *sums = stage_pass(1, second, ordered[1], sums)
    rows2, cots2, act, d_gate, d_up, *far = last_pass(third, gate_w, up_w, down_w[2], sums)
    far = (to_xy(far[0], 1), to_xy(far[1], -1), to_y(far[2], 2), to_xy(far[3], 2))
    near = near_pass(d_gate, d_up, gate_w, up_w)
    near = (near[3], to_y(near[0], 1), to_y(near[1], -1), to_x(near[2]))
    weight_grads = expert_weights_pass(
        (rows0, rows1, rows2), (cots0, cots1, cots2), act, d_gate, d_up
    )
    total = near[0].astype(F32)
    for part in (*far, *near[1:]):
        total = total + part.astype(F32)
    total = total.astype(BF16)
    returned = lax.all_to_all(total, ("z", "x"), 0, 0, tiled=True)
    resid_part = combine(returned.reshape(EXPERTS, 2, CAP, 256), places, own_cot)
    resid_pieces = (
        resid_part,
        to_y(resid_part, 1),
        to_y(resid_part, 2),
        to_y(resid_part, 3),
    )
    others = [to_c(other) for other in weight_grads[3:]]
    grad_gate, grad_up, grad_down = finish(weight_grads[:3], others)

    conv_vals = conv_out.astype(F32)
    sums = sum_over_y(
        jnp.stack([jnp.sum(conv_vals, axis=1), jnp.sum(conv_vals * conv_vals, axis=1)])
    )
    mean = sums[0][:, None] / DB
    rstd = lax.rsqrt(sums[1][:, None] / DB - mean * mean + 1e-05)
    normed = (conv_vals - mean) * rstd
    zpre = normed * norm_gain[None, :]
    zsig = jax.nn.sigmoid(zpre)
    mixed = (zpre * zsig).astype(BF16)

    resid_grad, keep, give = proj(resid_pieces, mixed)
    by_owner = (keep.astype(F32) + to_c(give).astype(F32)).astype(BF16)
    resid_grad, by_owner = lax.optimization_barrier((resid_grad, by_owner))
    owned = lax.all_to_all(by_owner, ("z", "x"), 0, 0, tiled=True)
    grad_proj = jnp.sum(owned.astype(F32), axis=0)

    d_norm, sums = channels(resid_grad, out_proj, normed, norm_gain[None, :])
    sums = sum_over_y(sums)
    conv_grad = (
        rstd * (d_norm - sums[0][:, None] / DB - normed * sums[1][:, None] / DB)
    ).astype(BF16)
    n_sp = NZ * NX * NC
    later_rows = lax.ppermute(conv_grad[: WIDTH - 1], SP, [(i, i - 1) for i in range(1, n_sp)])
    extended = jnp.concatenate([conv_grad, later_rows], axis=0).astype(F32)
    unit_grad = lax.conv_general_dilated(
        extended[None],
        taps[:, None, :],
        (1,),
        "VALID",
        dimension_numbers=("NWC", "WIO", "NWC"),
        feature_group_count=taps.shape[1],
        precision=lax.Precision.HIGHEST,
    )[0]
    gate_sig_in = jax.nn.sigmoid(glu_gate.astype(F32))
    grad_glu_value = (unit_grad * gate_sig_in).astype(BF16)
    grad_glu_gate = (
        unit_grad * glu_value.astype(F32) * gate_sig_in * (1.0 - gate_sig_in)
    ).astype(BF16)
    return (
        grad_gate.T[None],
        grad_up.T[None],
        grad_down[None],
        grad_proj,
        grad_glu_value,
        grad_glu_gate,
    )


def solution(mesh):
    wide = Mesh(mesh.devices.reshape(NZ, NX, NC, NY), ("z", "x", "c", "y"))
    in_specs = (
        P(SP, None),
        P(SP, None),
        P(SP, None),
        P(SP, None),
        P(SP, None, "y"),
        P(SP, None, "y"),
        P(SP, "y", None),
        P(None, "y"),
        P(SP, "y"),
        P(SP, "y"),
        P(SP, "y"),
        P(None, "y"),
        P("y"),
    )
    out_specs = (
        P(SP, None, "y"),
        P(SP, None, "y"),
        P(SP, "y", None),
        P(SP, "y"),
        P(SP, "y"),
        P(SP, "y"),
    )
    return jax.shard_map(step, mesh=wide, in_specs=in_specs, out_specs=out_specs, check_vma=False)
```

```python
import jax
import jax.numpy as jnp
from jax import lax
from jax.experimental import pallas as pl
from jax.experimental.pallas import tpu as pltpu
from jax.sharding import Mesh, PartitionSpec as P


DB = 1024
WIDTH = 31
EXPERTS = 16
CAP = 16
NZ, NX, NC, NY = 8, 4, 2, 4
ZX = NZ * NX
SP = ("z", "x", "c")
F32 = jnp.float32
BF16 = jnp.bfloat16


BIG = pltpu.CompilerParams(vmem_limit_bytes=20 * 2**20)
SMALL = pltpu.CompilerParams(vmem_limit_bytes=10 * 2**20)
VMEM = pl.BlockSpec(memory_space=pltpu.VMEM)
HBM = pl.BlockSpec(memory_space=pl.ANY)
CONTRACT_FIRST = (((0,), (0,)), ((), ()))
CONTRACT_LAST = (((1,), (1,)), ((), ()))


def to_y(v, d):
    return lax.ppermute(v, "y", [(i, (i + d) % NY) for i in range(NY)])


def to_x(v):
    return lax.ppermute(v, "x", [(i, i ^ 1) for i in range(NX)])


def to_c(v):
    return lax.ppermute(v, "c", [(0, 1), (1, 0)])


def swish_slope(pre, sig):
    return sig * (1.0 + pre * (1.0 - sig))


def own_col(dx, dy):
    block = lax.rem(lax.axis_index("y") + dy, NY)
    return 256 * (2 * block + lax.rem(lax.axis_index("x") + dx, 2))


def own_quarter():
    return pl.ds(pl.multiple_of(512 * lax.axis_index("y"), 512), 512)


def prep_body(routes, weights, all_rows, all_cots, send, places, own_cot, rows, cots, sems):
    copies = [
        pltpu.make_async_copy(src.at[:, own_quarter()], dst, sems.at[i])
        for i, (src, dst) in enumerate(((all_rows, rows), (all_cots, cots)))
    ]
    for copy in copies:
        copy.start()
    lane = lax.broadcasted_iota(jnp.int32, (EXPERTS, 128), 0)
    first = (lane == routes[0:1, :]).astype(F32)
    second = (lane == routes[1:2, :]).astype(F32)
    before = (
        lax.broadcasted_iota(jnp.int32, (128, 128), 0)
        < lax.broadcasted_iota(jnp.int32, (128, 128), 1)
    ).astype(BF16)
    earlier = jnp.dot((first + second).astype(BF16), before, preferred_element_type=F32)
    slot0 = jnp.sum(earlier * first, axis=0, keepdims=True).astype(jnp.int32)
    slot1 = jnp.sum(earlier * second, axis=0, keepdims=True).astype(jnp.int32)
    place = lax.broadcasted_iota(jnp.int32, (EXPERTS * CAP, 128), 0)
    hit0 = place == routes[0:1, :] * CAP + slot0
    hit1 = place == routes[1:2, :] * CAP + slot1
    scale = jnp.sum(
        jnp.where(hit0, weights[0:1, :], 0.0) + jnp.where(hit1, weights[1:2, :], 0.0),
        axis=1,
        keepdims=True,
    )
    pick = jnp.where(hit0 | hit1, 1.0, 0.0).astype(BF16)
    places[...] = pick
    for copy in copies:
        copy.wait()
    own_cot[...] = cots[...]
    sent_rows = jnp.dot(pick, rows[...], preferred_element_type=F32).astype(BF16)
    sent_cots = (scale * jnp.dot(pick, cots[...], preferred_element_type=F32)).astype(BF16)
    for half in range(2):
        cols = slice(256 * half, 256 * half + 256)
        send[:, half, 0] = sent_rows[:, cols].reshape(EXPERTS, CAP, 256)
        send[:, half, 1] = sent_cots[:, cols].reshape(EXPERTS, CAP, 256)


def prep(routes, weights, rows, cots):
    return pl.pallas_call(
        prep_body,
        out_shape=(
            jax.ShapeDtypeStruct((EXPERTS, 2, 2, CAP, 256), BF16),
            jax.ShapeDtypeStruct((EXPERTS * CAP, 128), BF16),
            jax.ShapeDtypeStruct((128, 512), BF16),
        ),
        in_specs=[VMEM, VMEM, HBM, HBM],
        out_specs=(VMEM,) * 3,
        scratch_shapes=[
            pltpu.VMEM((128, 512), BF16),
            pltpu.VMEM((128, 512), BF16),
            pltpu.SemaphoreType.DMA((2,)),
        ],
        name="prep",
    )(routes, weights, rows, cots)


BLOCKS = ((0, 0), (0, 3), (0, 1), (1, 0), (1, 3), (1, 1), (0, 2), (1, 2))
STAGES = ((0, 4), (4, 7), (7, 8))
HALF = ZX // 2
LAYOUTS = (
    ((0, 0, ZX), (1, 0, ZX), (2, 0, ZX), (3, 0, ZX)),
    ((0, 0, ZX), (1, 0, ZX), (2, 0, ZX)),
    ((0, 0, HALF), (0, HALF, HALF)),
)


def gather_first(v):
    return v, to_y(v, 1), to_y(v, -1), to_x(v)


def gather_second(first):
    _, behind, _, beside = first
    return to_x(behind), to_y(beside, -1), to_y(behind, 1)


def gather_third(second):
    return to_y(second[0][:HALF], 1), to_y(second[1][HALF:], -1)


def weights_in_order_body(*refs):
    for i in range(3):
        for stage, (lo, hi) in enumerate(STAGES):
            out = refs[6 + 3 * i + stage]
            for block in range(lo, hi):
                at = pl.ds(pl.multiple_of(own_col(*BLOCKS[block]), 256), 256)
                cols = slice(256 * (block - lo), 256 * (block - lo + 1))
                for side in range(2):
                    out[224 * side : 224 * side + 224, cols] = refs[2 * i + side][:, at]


def weights_in_order(flat):
    out = tuple(jax.ShapeDtypeStruct((448, 256 * (hi - lo)), BF16) for lo, hi in STAGES)
    res = pl.pallas_call(
        weights_in_order_body,
        out_shape=out * 3,
        in_specs=[VMEM] * 6,
        out_specs=(VMEM,) * 9,
        compiler_params=BIG,
        name="weights_in_order",
    )(*flat)
    return [(res[s], res[3 + s], res[6 + s]) for s in range(3)]


def put_pieces(pieces, layout, rows, cots):
    for piece, (block, first, count) in zip(pieces, layout):
        cols = slice(256 * block, 256 * block + 256)
        span = slice(first * CAP, (first + count) * CAP)
        rows[span, cols] = piece[:, 0].reshape(count * CAP, 256)
        cots[span, cols] = piece[:, 1].reshape(count * CAP, 256)


def stage_pass(stage, pieces, weights, before):
    layout = LAYOUTS[stage]
    n = len(layout)
    width = 256 * (STAGES[stage][1] - STAGES[stage][0])

    def body(*refs):
        given = refs[n + 3 : n + 3 + len(before)]
        rows, cots, *sums = refs[n + 3 + len(before) :]
        put_pieces(refs[:n], layout, rows, cots)
        for i, left in enumerate((rows, rows, cots)):
            part = lax.dot_general(
                left[...], refs[n + i][...], CONTRACT_LAST, preferred_element_type=F32
            )
            sums[i][...] = part + given[i][...] if before else part

    return pl.pallas_call(
        body,
        out_shape=(jax.ShapeDtypeStruct((ZX * CAP, width), BF16),) * 2
        + (jax.ShapeDtypeStruct((ZX * CAP, 448), F32),) * 3,
        in_specs=[VMEM] * (n + 3 + len(before)),
        out_specs=(VMEM,) * 5,
        input_output_aliases={n + 3 + i: 2 + i for i in range(len(before))},
        compiler_params=BIG,
    )(*pieces, *weights, *before)


def weights_of(block, gates):
    stage = next(s for s, (lo, hi) in enumerate(STAGES) if lo <= block < hi)
    at = 256 * (block - STAGES[stage][0])
    return gates[stage][:, at : at + 256]


def row_grads(d_gate, d_up, gate_w, up_w, blocks, grads):
    for block, grad in zip(blocks, grads):
        part = jnp.dot(
            d_gate[...], weights_of(block, gate_w), preferred_element_type=F32
        ) + jnp.dot(d_up[...], weights_of(block, up_w), preferred_element_type=F32)
        grad[...] = part.astype(BF16).reshape(ZX, CAP, 256)


FAR = (5, 4, 7, 3)
NEAR = (2, 1, 6, 0)


def last_body(*refs):
    pieces = refs[:2]
    gate_w, up_w, down_w = refs[2:5], refs[5:8], refs[8]
    before = refs[9:12]
    rows, cots, act, d_gate, d_up = refs[12:17]
    put_pieces(pieces, LAYOUTS[2], rows, cots)

    @pl.loop(0, 2)
    def _(m):
        span = pl.ds(pl.multiple_of(256 * m, 256), 256)
        gate, up, d_act = [
            before[i][span]
            + lax.dot_general(left[span], w[...], CONTRACT_LAST, preferred_element_type=F32)
            for i, (left, w) in enumerate(((rows, gate_w[2]), (rows, up_w[2]), (cots, down_w)))
        ]
        sig = jax.nn.sigmoid(gate)
        silu = gate * sig
        act[span] = (silu * up).astype(BF16)
        d_gate[span] = (d_act * up * swish_slope(gate, sig)).astype(BF16)
        d_up[span] = (d_act * silu).astype(BF16)

    row_grads(d_gate, d_up, gate_w, up_w, FAR, refs[17:21])


def last_pass(pieces, gate_w, up_w, down_w, before):
    n = ZX * CAP
    return pl.pallas_call(
        last_body,
        out_shape=(jax.ShapeDtypeStruct((n, 256), BF16),) * 2
        + (jax.ShapeDtypeStruct((n, 448), BF16),) * 3
        + (jax.ShapeDtypeStruct((ZX, CAP, 256), BF16),) * 4,
        in_specs=[VMEM] * 12,
        out_specs=(VMEM,) * 9,
        compiler_params=BIG,
        name="last_stage",
    )(*pieces, *gate_w, *up_w, down_w, *before)


def near_body(*refs):
    row_grads(refs[0], refs[1], refs[2:5], refs[5:8], NEAR, refs[8:12])


def near_pass(d_gate, d_up, gate_w, up_w):
    return pl.pallas_call(
        near_body,
        out_shape=(jax.ShapeDtypeStruct((ZX, CAP, 256), BF16),) * 4,
        in_specs=[VMEM] * 8,
        out_specs=(VMEM,) * 4,
        compiler_params=BIG,
        name="near_rows",
    )(d_gate, d_up, *gate_w, *up_w)


def add_up(parts):
    def body(*refs):
        total = refs[0][...].astype(F32)
        for part in refs[1:-1]:
            total = total + part[...].astype(F32)
        refs[-1][...] = total.astype(BF16)

    return pl.pallas_call(
        body,
        out_shape=jax.ShapeDtypeStruct((ZX, CAP, 256), BF16),
        in_specs=[VMEM] * len(parts),
        out_specs=VMEM,
        compiler_params=SMALL,
    )(*parts)


def weights_body(*refs):
    rows, cots = refs[0:3], refs[3:6]
    act, d_gate, d_up = refs[6:9]
    outs = refs[9:15]
    turned = refs[15]
    half = 224
    for i, (left, rights) in enumerate(((d_gate, rows), (d_up, rows), (act, cots))):
        turned[...] = left[...].T
        for stage, (lo, hi) in enumerate(STAGES):
            for block in range(lo, hi):
                at = slice(256 * (block - lo), 256 * (block - lo + 1))
                grad = jnp.dot(turned[...], rights[stage][:, at], preferred_element_type=F32)
                grad = grad.astype(BF16)
                to = pl.ds(pl.multiple_of(own_col(*BLOCKS[block]), 256), 256)
                outs[i][:, to] = grad[:half]
                outs[3 + i][:, to] = grad[half:]


def expert_weights_pass(rows, cots, act, d_gate, d_up):
    out = jax.ShapeDtypeStruct((act.shape[1] // 2, 2048), BF16)
    return pl.pallas_call(
        weights_body,
        out_shape=(out,) * 6,
        in_specs=[VMEM] * 9,
        out_specs=(VMEM,) * 6,
        scratch_shapes=[pltpu.VMEM((448, ZX * CAP), BF16)],
        compiler_params=BIG,
        name="expert_weights",
    )(*rows, *cots, act, d_gate, d_up)


def finish_body(*refs):
    for i in range(3):
        total = refs[i][...].astype(F32) + refs[3 + i][...].astype(F32)
        refs[6 + i][...] = total.astype(BF16)


def finish(own, others):
    out = jax.ShapeDtypeStruct(own[0].shape, BF16)
    return pl.pallas_call(
        finish_body,
        out_shape=(out,) * 3,
        in_specs=[VMEM] * 6,
        out_specs=(VMEM,) * 3,
        compiler_params=BIG,
        name="finish",
    )(*own, *others)


def combine_body(returned, places, cot, out):
    for half in range(2):
        cols = slice(256 * half, 256 * half + 256)
        slots = returned[:, half].reshape(EXPERTS * CAP, 256)
        moe = lax.dot_general(places[...], slots, CONTRACT_FIRST, preferred_element_type=F32)
        out[:, cols] = (cot[:, cols].astype(F32) + moe).astype(BF16)


def combine(returned, places, cot):
    return pl.pallas_call(
        combine_body,
        out_shape=jax.ShapeDtypeStruct(cot.shape, BF16),
        in_specs=[VMEM] * 3,
        out_specs=VMEM,
        compiler_params=SMALL,
        name="combine",
    )(returned, places, cot)


def proj_body(own, one, two, three, mixed, resid, keep, send, table):
    y = lax.axis_index("y")
    for d, piece in enumerate((own, one, two, three)):
        block = lax.rem(y + (NY - d), NY)
        resid[:, pl.ds(pl.multiple_of(block * 512, 512), 512)] = piece[...]
        part = lax.dot_general(piece[...], mixed[...], CONTRACT_FIRST, preferred_element_type=F32)
        table[pl.ds(block * 8, 8)] = part.astype(BF16).reshape(8, 2, 32, 256)
    core = lax.axis_index("c")
    keep[...] = table[:, core]
    send[...] = table[:, 1 - core]


def proj(pieces, mixed):
    return pl.pallas_call(
        proj_body,
        out_shape=(
            jax.ShapeDtypeStruct((128, 2048), BF16),
            jax.ShapeDtypeStruct((ZX, 32, 256), BF16),
            jax.ShapeDtypeStruct((ZX, 32, 256), BF16),
        ),
        in_specs=[VMEM] * 5,
        out_specs=(VMEM,) * 3,
        scratch_shapes=[pltpu.VMEM((ZX, 2, 32, 256), BF16)],
        compiler_params=SMALL,
        name="proj",
    )(*pieces, mixed)


def channels_body(resid, out_proj, normed, gain, d_norm, sums):
    d_mixed = jnp.dot(resid[...], out_proj[...], preferred_element_type=F32)
    zpre = normed[...] * gain[...]
    grad = d_mixed * swish_slope(zpre, jax.nn.sigmoid(zpre)) * gain[...]
    d_norm[...] = grad
    first = jnp.sum(grad, axis=1, keepdims=True)
    second = jnp.sum(grad * normed[...], axis=1, keepdims=True)
    lane = lax.broadcasted_iota(jnp.int32, (128, 128), 1)
    table = jnp.where(lane == 0, first, jnp.where(lane == 1, second, 0.0))
    sums[...] = table.T[0:8]


def channels(resid, out_proj, normed, gain):
    return pl.pallas_call(
        channels_body,
        out_shape=(
            jax.ShapeDtypeStruct(normed.shape, F32),
            jax.ShapeDtypeStruct((8, 128), F32),
        ),
        in_specs=[VMEM] * 4,
        out_specs=(VMEM,) * 2,
        compiler_params=SMALL,
        name="channels",
    )(resid, out_proj, normed, gain)


def sum_over_y(v):
    return v + to_y(v, 1) + to_y(v, -1) + to_y(v, 2)


def step(
    moe_input,
    out_cotangent,
    routes,
    route_weight,
    w_gate,
    w_up,
    w_down,
    out_proj,
    conv_out,
    glu_value,
    glu_gate,
    taps,
    norm_gain,
):
    send, places, own_cot = prep(routes.T, route_weight.T, moe_input, out_cotangent)
    shard = lax.all_to_all(send.reshape(ZX, 2, CAP, 256), ("z", "x"), 0, 0, tiled=True)
    own_w = (w_gate[0].T, w_up[0].T, w_down[0])
    ordered = weights_in_order([v for w in own_w for v in (w, to_c(w))])
    shard, ordered = lax.optimization_barrier((shard, ordered))
    gate_w, up_w, down_w = zip(*ordered)
    first = gather_first(shard)
    second = gather_second(first)
    rows0, cots0, *sums = stage_pass(0, first, ordered[0], ())
    third = gather_third(second)
    rows1, cots1, *sums = stage_pass(1, second, ordered[1], sums)
    rows2, cots2, act, d_gate, d_up, *far = last_pass(third, gate_w, up_w, down_w[2], sums)
    side = (to_y(far[0], 1), to_y(far[1], -1), to_x(far[2]))
    near = near_pass(d_gate, d_up, gate_w, up_w)
    near_arrived = (to_y(near[0], 1), to_y(near[1], -1))
    beside = add_up((far[3], side[0], side[1]))
    opposite = add_up((near[2], side[2]))
    last_arrived = (to_x(beside), to_y(opposite, 2))
    weight_grads = expert_weights_pass(
        (rows0, rows1, rows2), (cots0, cots1, cots2), act, d_gate, d_up
    )
    total = near[3].astype(F32)
    for part in (*near_arrived, *last_arrived):
        total = total + part.astype(F32)
    total = total.astype(BF16)
    returned = lax.all_to_all(total, ("z", "x"), 0, 0, tiled=True)
    resid_part = combine(returned.reshape(EXPERTS, 2, CAP, 256), places, own_cot)
    resid_pieces = (
        resid_part,
        to_y(resid_part, 1),
        to_y(resid_part, 2),
        to_y(resid_part, 3),
    )
    others = [to_c(other) for other in weight_grads[3:]]
    grad_gate, grad_up, grad_down = finish(weight_grads[:3], others)

    conv_vals = conv_out.astype(F32)
    sums = sum_over_y(
        jnp.stack([jnp.sum(conv_vals, axis=1), jnp.sum(conv_vals * conv_vals, axis=1)])
    )
    mean = sums[0][:, None] / DB
    rstd = lax.rsqrt(sums[1][:, None] / DB - mean * mean + 1e-05)
    normed = (conv_vals - mean) * rstd
    zpre = normed * norm_gain[None, :]
    zsig = jax.nn.sigmoid(zpre)
    mixed = (zpre * zsig).astype(BF16)

    resid_grad, keep, give = proj(resid_pieces, mixed)
    by_owner = (keep.astype(F32) + to_c(give).astype(F32)).astype(BF16)
    resid_grad, by_owner = lax.optimization_barrier((resid_grad, by_owner))
    owned = lax.all_to_all(by_owner, ("z", "x"), 0, 0, tiled=True)
    grad_proj = jnp.sum(owned.astype(F32), axis=0)

    d_norm, sums = channels(resid_grad, out_proj, normed, norm_gain[None, :])
    sums = sum_over_y(sums)
    conv_grad = (
        rstd * (d_norm - sums[0][:, None] / DB - normed * sums[1][:, None] / DB)
    ).astype(BF16)
    n_sp = NZ * NX * NC
    later_rows = lax.ppermute(conv_grad[: WIDTH - 1], SP, [(i, i - 1) for i in range(1, n_sp)])
    extended = jnp.concatenate([conv_grad, later_rows], axis=0).astype(F32)
    unit_grad = lax.conv_general_dilated(
        extended[None],
        taps[:, None, :],
        (1,),
        "VALID",
        dimension_numbers=("NWC", "WIO", "NWC"),
        feature_group_count=taps.shape[1],
        precision=lax.Precision.HIGHEST,
    )[0]
    gate_sig_in = jax.nn.sigmoid(glu_gate.astype(F32))
    grad_glu_value = (unit_grad * gate_sig_in).astype(BF16)
    grad_glu_gate = (
        unit_grad * glu_value.astype(F32) * gate_sig_in * (1.0 - gate_sig_in)
    ).astype(BF16)
    return (
        grad_gate.T[None],
        grad_up.T[None],
        grad_down[None],
        grad_proj,
        grad_glu_value,
        grad_glu_gate,
    )


def solution(mesh):
    wide = Mesh(mesh.devices.reshape(NZ, NX, NC, NY), ("z", "x", "c", "y"))
    in_specs = (
        P(SP, None),
        P(SP, None),
        P(SP, None),
        P(SP, None),
        P(SP, None, "y"),
        P(SP, None, "y"),
        P(SP, "y", None),
        P(None, "y"),
        P(SP, "y"),
        P(SP, "y"),
        P(SP, "y"),
        P(None, "y"),
        P("y"),
    )
    out_specs = (
        P(SP, None, "y"),
        P(SP, None, "y"),
        P(SP, "y", None),
        P(SP, "y"),
        P(SP, "y"),
        P(SP, "y"),
    )
    return jax.shard_map(step, mesh=wide, in_specs=in_specs, out_specs=out_specs, check_vma=False)
```
